32 devices in a mesh: sp: 16 (over z, y, core), tp: 2 (over x).
Axes of the slice: x: 2, y: 2, z: 4, core: 2. Of those that a mesh axis runs over, the one named last changes fastest.
Arguments:
- tokens: bfloat16 [12288, 2048], P(('sp', 'tp')), may hold values from -6 to 6
- input_norm_gain: bfloat16 [2048], replicated, may hold values from 0.099609375 to 1.8984375
- convolution_outer_weight: bfloat16 [2048, 1024], P(None, 'tp'), may hold values from -0.125 to 0.125
- convolution_inner_weight: bfloat16 [2048, 1024], P(None, 'tp'), may hold values from -0.125 to 0.125
- convolution_signal_weight: bfloat16 [2048, 1024], P(None, 'tp'), may hold values from -0.125 to 0.125
- convolution_kernel_taps: bfloat16 [3, 1024], replicated, may hold values from -3.5 to 3.5
- memory_query_matrix: bfloat16 [2048, 512], P(None, 'tp'), may hold values from -0.125 to 0.125
- memory_key_matrix: bfloat16 [2048, 512], P(None, 'tp'), may hold values from -0.125 to 0.125
- memory_value_matrix: bfloat16 [2048, 1024], P(None, 'tp'), may hold values from -0.125 to 0.125
- output_gate_weight: bfloat16 [2048, 1024], P(None, 'tp'), may hold values from -0.125 to 0.125
- input_gate_weight: bfloat16 [2048, 8], replicated, may hold values from -0.5 to 0.5
- forget_gate_weight: bfloat16 [2048, 8], replicated, may hold values from -0.125 to 0.125
- input_gate_bias: float32 [8], replicated, may hold values from -1 to 125
- forget_gate_bias: float32 [8], replicated, may hold values from 3.5 to 12.5
- position_forget_factor: float32 [12288], P('sp'), may hold values from 0.5 to 2
- extra_log_decay: float32 [12288, 8], P('sp'), may hold values from -0.7 to 0
- starting_memory_state: float32 [8, 64, 128], replicated, may hold values from -6 to 6
- starting_log_scale: float32 [8], replicated, may hold values from 5 to 125
- head_norm_gain: bfloat16 [1024], replicated, may hold values from 0.099609375 to 1.8984375
- convolution_output_weight: bfloat16 [1024, 2048], P('tp'), may hold values from -0.125 to 0.125
- memory_output_weight: bfloat16 [1024, 2048], P('tp'), may hold values from -0.125 to 0.125
Outputs:
- mixed: bfloat16 [12288, 2048], P(('sp', 'tp'))
The draws below stay inside these ranges and needn't reach their ends.
All inputs are finite; a program needn't handle non-finite values.
Results may differ from the reference program's by a relative error of at most 0.035.
Values may be sent and summed in bfloat16 or wider, within the bound.
A program may use at most 64 MiB of HBM per device.

```python
import jax
import jax.numpy as jnp
from jax import lax

D = 2048
CONV = 1024
WIDTH = 3
MH = 8
DQK = 64
DV = 128
SPAN = 128
TOKENS = 12288
N_TP = 2


def draw_input_gate_bias(key, part):
    return jax.random.uniform(key, (MH,), jnp.float32, -1.0, 1.0)


def draw_forget_gate_bias(key, part):
    order_key = jax.random.fold_in(key, 11)
    level_key = jax.random.fold_in(key, 12)
    ranking = jax.random.permutation(order_key, MH)
    slow_count = MH // 2
    jitter = jax.random.uniform(level_key, (MH,), jnp.float32, 0.0, 1.0)
    return jnp.where(ranking < slow_count, 11.5 + jitter, 3.5 + jitter)


def draw_position_forget_factor(key, part):
    levels = jnp.exp(jax.random.uniform(key, (TOKENS // SPAN,), jnp.float32, jnp.log(0.5), jnp.log(2.0)))
    return jnp.repeat(levels, SPAN)


def draw_extra_log_decay(key, part):
    place_key = jax.random.fold_in(key, 21)
    size_key = jax.random.fold_in(key, 22)
    spots = jax.random.randint(place_key, (2, MH), 0, TOKENS)
    amounts = jnp.log(jax.random.uniform(size_key, (2, MH), jnp.float32, 0.5, 0.8))
    positions = jnp.arange(TOKENS, dtype=jnp.int32)[:, None, None]
    hits = positions == spots[None]
    return jnp.sum(jnp.where(hits, amounts[None], 0.0), axis=1)


def draw_starting_log_scale(key, part):
    return jax.random.uniform(key, (MH,), jnp.float32, 9.0, 12.0)


def shard_levels(own_key, extent, shards, low, top_value):
    factor_of = 1.0
    for position, blocks in shards:
        heights = jax.random.uniform(jax.random.fold_in(jax.random.fold_in(own_key, 6), position), (blocks,), jnp.float32, low / len(shards), top_value / len(shards))
        factor_of = factor_of * jnp.repeat(jnp.exp(heights), extent[position] // blocks).reshape((-1,) + (1,) * (len(extent) - 1 - position))
    return factor_of


def gaussian(stream_key, dims, width, limit, cuts=(), kind=jnp.bfloat16):
    drawn = jax.random.normal(stream_key, dims, jnp.float32) * width
    if len(cuts) > 0:
        drawn = shard_levels(stream_key, dims, cuts, -0.22, 0.18) * drawn
    return jnp.clip(drawn, min=-limit, max=limit).astype(kind)


def setup_inputs(seed: int = 0) -> dict:
    splits = jax.random.split(jax.random.key(seed), 22)
    return {
        "tokens": gaussian(splits[0], (TOKENS, D), 1.0, 6.0, ((0, 32),)),
        "input_norm_gain": jnp.clip(1.0 + 0.18 * jax.random.normal(splits[1], (D,), jnp.float32), 0.099609375, 1.8984375).astype(jnp.bfloat16),
        "convolution_outer_weight": gaussian(splits[2], (D, CONV), D ** -0.5, 0.125, ((1, 2),)),
        "convolution_inner_weight": gaussian(splits[3], (D, CONV), D ** -0.5, 0.125, ((1, 2),)),
        "convolution_signal_weight": gaussian(splits[4], (D, CONV), D ** -0.5, 0.125, ((1, 2),)),
        "convolution_kernel_taps": gaussian(splits[5], (WIDTH, CONV), WIDTH ** -0.5, 3.5),
        "memory_query_matrix": gaussian(splits[6], (D, MH * DQK), D ** -0.5, 0.125, ((1, 2),)),
        "memory_key_matrix": gaussian(splits[7], (D, MH * DQK), D ** -0.5, 0.125, ((1, 2),)),
        "memory_value_matrix": gaussian(splits[8], (D, MH * DV), D ** -0.5, 0.125, ((1, 2),)),
        "output_gate_weight": gaussian(splits[9], (D, MH * DV), D ** -0.5, 0.125, ((1, 2),)),
        "input_gate_weight": gaussian(splits[10], (D, MH), (D // 16) ** -0.5, 0.5),
        "forget_gate_weight": gaussian(splits[11], (D, MH), D ** -0.5, 0.125),
        "input_gate_bias": draw_input_gate_bias(jax.random.fold_in(splits[21], 71), 0),
        "forget_gate_bias": draw_forget_gate_bias(jax.random.fold_in(splits[21], 71), 0),
        "position_forget_factor": draw_position_forget_factor(jax.random.fold_in(splits[21], 71), 0),
        "extra_log_decay": draw_extra_log_decay(jax.random.fold_in(splits[21], 71), 0),
        "starting_memory_state": gaussian(splits[16], (MH, DQK, DV), 1.0, 6.0, (), jnp.float32),
        "starting_log_scale": draw_starting_log_scale(jax.random.fold_in(splits[21], 71), 0),
        "head_norm_gain": jnp.clip(1.0 + 0.18 * jax.random.normal(splits[18], (MH * DV,), jnp.float32), 0.099609375, 1.8984375).astype(jnp.bfloat16),
        "convolution_output_weight": gaussian(splits[19], (CONV, D), (CONV + MH * DV) ** -0.5, 0.125, ((0, 2),)),
        "memory_output_weight": gaussian(splits[20], (MH * DV, D), (CONV + MH * DV) ** -0.5, 0.125, ((0, 2),)),
    }


EPS = 1e-06
HIGHEST_PRECISION = lax.Precision.HIGHEST

def merge_states(earlier, later):
    state_one, peak_one, decay_one = earlier
    state_two, peak_two, decay_two = later
    lifted = peak_one + decay_two
    ceiling = jnp.maximum(lifted, peak_two)
    merged = jnp.exp(lifted - ceiling)[..., None, None] * state_one + jnp.exp(peak_two - ceiling)[..., None, None] * state_two
    return (merged, ceiling, decay_one + decay_two)

def block_terms(key_blocks, value_blocks, input_blocks, forget_blocks):
    cumulative = jnp.cumsum(forget_blocks, axis=2)
    block_total = cumulative[:, :, -1]
    weight_log = block_total[:, :, None] - cumulative + input_blocks
    block_peak = lax.optimization_barrier(jnp.max(weight_log, axis=2))
    weights = jnp.exp(weight_log - block_peak[:, :, None])
    block_state = jnp.einsum('nhld,nhle->nhde', key_blocks * weights[..., None], value_blocks, precision=HIGHEST_PRECISION)
    return (cumulative, block_state, block_peak, block_total)

def block_outputs(query_blocks, key_blocks, value_blocks, input_blocks, cumulative, start_state, start_peak):
    span_len = query_blocks.shape[2]
    carried = cumulative + start_peak[:, :, None]
    pair_log = cumulative[:, :, :, None] - cumulative[:, :, None, :] + input_blocks[:, :, None, :]
    causal = jnp.tril(jnp.ones((span_len, span_len), dtype=bool))
    pair_log = jnp.where(causal, pair_log, -jnp.inf)
    ceiling = jnp.maximum(carried, lax.optimization_barrier(jnp.max(pair_log, axis=3)))
    scores = jnp.einsum('nhtd,nhsd->nhts', query_blocks, key_blocks, precision=HIGHEST_PRECISION) * jnp.exp(pair_log - ceiling[..., None])
    local_part = jnp.einsum('nhts,nhse->nhte', scores, value_blocks, precision=HIGHEST_PRECISION)
    remote = jnp.einsum('nhtd,nhde->nhte', query_blocks, start_state, precision=HIGHEST_PRECISION)
    return jnp.exp(carried - ceiling)[..., None] * remote + local_part

def reference(tokens, input_norm_gain, convolution_outer_weight, convolution_inner_weight, convolution_signal_weight, convolution_kernel_taps, memory_query_matrix, memory_key_matrix, memory_value_matrix, output_gate_weight, input_gate_weight, forget_gate_weight, input_gate_bias, forget_gate_bias, position_forget_factor, extra_log_decay, starting_memory_state, starting_log_scale, head_norm_gain, convolution_output_weight, memory_output_weight):
    row_count = tokens.shape[0]
    widened = tokens.astype(jnp.float32)
    normed = (widened * lax.rsqrt(lax.optimization_barrier(jnp.mean(widened * widened, axis=1, keepdims=True)) + EPS) * input_norm_gain.astype(jnp.float32)).astype(jnp.bfloat16)

    def project(weight):
        return jnp.dot(normed, weight, preferred_element_type=jnp.float32).astype(jnp.bfloat16)
    outer_gate = project(convolution_outer_weight)
    inner_gate = project(convolution_inner_weight)
    signal = project(convolution_signal_weight)
    mixed_in = inner_gate.astype(jnp.float32) * signal.astype(jnp.float32)
    tap_count = convolution_kernel_taps.shape[0]
    padded = jnp.pad(mixed_in, ((tap_count - 1, 0), (0, 0)))
    conv_sum = jnp.zeros((row_count, CONV), jnp.float32)
    for offset in range(tap_count):
        conv_sum = conv_sum + convolution_kernel_taps[offset].astype(jnp.float32) * padded[offset:offset + row_count]
    conv_out = (outer_gate.astype(jnp.float32) * conv_sum).astype(jnp.bfloat16)
    queries = project(memory_query_matrix)
    key_rows = project(memory_key_matrix)
    value_rows = project(memory_value_matrix)
    out_gate = project(output_gate_weight)
    log_input = jnp.dot(normed, input_gate_weight, preferred_element_type=jnp.float32) + input_gate_bias
    forget_preactivation = jnp.dot(normed, forget_gate_weight, preferred_element_type=jnp.float32) + forget_gate_bias
    forget_log_values = position_forget_factor[:, None] * jax.nn.log_sigmoid(forget_preactivation) + extra_log_decay
    block_count = row_count // SPAN

    def heads_first(source, column_width):
        return source.astype(jnp.float32).reshape(block_count, SPAN, MH, column_width).transpose(0, 2, 1, 3)

    def gates_first(source):
        return source.reshape(block_count, SPAN, MH).transpose(0, 2, 1)
    query_blocks = heads_first(queries, DQK) * DQK ** (-0.5)
    key_blocks = heads_first(key_rows, DQK)
    value_blocks = heads_first(value_rows, DV)
    input_blocks = gates_first(log_input)
    forget_blocks = gates_first(forget_log_values)
    cumulative, block_state, block_peak, block_total = block_terms(key_blocks, value_blocks, input_blocks, forget_blocks)

    def advance(carried_state, block_item):
        return (merge_states(carried_state, block_item), carried_state[:2])
    start_tuple = (starting_memory_state, starting_log_scale, jnp.zeros((MH,), jnp.float32))
    final_state, starts = lax.scan(advance, start_tuple, (block_state, block_peak, block_total))
    numerator = block_outputs(query_blocks, key_blocks, value_blocks, input_blocks, cumulative, starts[0], starts[1])
    numerator = numerator.transpose(0, 2, 1, 3).reshape(row_count, MH, DV)
    normal_rows = numerator * lax.rsqrt(lax.optimization_barrier(jnp.mean(numerator * numerator, axis=2, keepdims=True)) + EPS)
    memory_out = (normal_rows.reshape(row_count, MH * DV) * head_norm_gain.astype(jnp.float32) * jax.nn.sigmoid(out_gate.astype(jnp.float32))).astype(jnp.bfloat16)
    conv_width = CONV // N_TP
    memory_width = MH * DV // N_TP
    summed = jnp.zeros((row_count, D), jnp.float32)
    for group_index in range(N_TP):
        conv_lo = group_index * conv_width
        memory_lo = group_index * memory_width
        group_term = jnp.dot(conv_out[:, conv_lo:conv_lo + conv_width], convolution_output_weight[conv_lo:conv_lo + conv_width], preferred_element_type=jnp.float32) + jnp.dot(memory_out[:, memory_lo:memory_lo + memory_width], memory_output_weight[memory_lo:memory_lo + memory_width], preferred_element_type=jnp.float32)
        summed = summed + lax.optimization_barrier(group_term.astype(jnp.bfloat16)).astype(jnp.float32)
    return summed.astype(jnp.bfloat16)
```

```python
import functools

import jax
import jax.numpy as jnp
from jax import lax
from jax.experimental import pallas as pl
from jax.experimental.pallas import tpu as pltpu
from jax.sharding import PartitionSpec as P

DQK = 64
DV = 128
EPS = 1e-06
FLOOR_LOG = -1e30
MESH = pl.DeviceIdType.MESH
BF = jnp.bfloat16
F32 = jnp.float32


def scan_lanes(x, op, fill):
    width = x.shape[1]
    lane = lax.broadcasted_iota(jnp.int32, x.shape, 1)
    shift = 1
    while shift < width:
        x = op(x, jnp.where(lane >= shift, pltpu.roll(x, shift, 1), fill))
        shift *= 2
    return x


def merge(earlier, later):
    s1, p1, d1 = earlier
    s2, p2, d2 = later
    lifted = p1 + d2
    top = jnp.maximum(lifted, p2)
    w1 = jnp.exp(lifted - top)
    w2 = jnp.exp(p2 - top)
    return ([w1[h : h + 1] * s1[h] + w2[h : h + 1] * s2[h] for h in range(len(s1))], top, d1 + d2)


def kernel(
    n_sp, n_tp,
    tok, gain, wo, wi, ws, taps, wq, wk, wv, wg, gin, gfo, bin_, bfo, pos, extra, s0, p0, hgain, wco, wmo,
    out,
    rows, vo, vi, vs, vq, vk, vv, vg, vco, vmo,
    ao, mix, aq, ak, av, ag, gates, gates_t, own_t, own_c, local, halo_send,
    st_send, st_recv, sc_send, sc_recv, start_s, start_p, part_send, part_recv,
    wsem, tsend, trecv, hsem, ssend, srecv, psend, precv,
):
    me = lax.axis_index("tp")
    sq = lax.axis_index("sp")
    own = tok.shape[0]
    total = rows.shape[0]
    ch = 128 if own % 128 == 0 else own
    nch = own // ch
    heads = aq.shape[1] // DQK
    mh = gin.shape[1]
    cw = ao.shape[1]
    rounds = n_sp.bit_length() - 1

    pairs = [(wo, vo), (wi, vi), (ws, vs), (wq, vq), (wk, vk), (wv, vv), (wg, vg), (wco, vco), (wmo, vmo)]
    loads = [pltpu.make_async_copy(src, dst, wsem.at[i]) for i, (src, dst) in enumerate(pairs)]
    for load in loads:
        load.start()

    def partner(r):
        bit = (sq // (1 << r)) % 2
        return bit, sq + (1 - 2 * bit) * (1 << r)

    barrier = pltpu.get_barrier_semaphore()
    for k in range(1, n_tp):
        pl.semaphore_signal(barrier, inc=1, device_id={"tp": lax.rem(me + k, n_tp)}, device_id_type=MESH)
    for r in range(rounds):
        pl.semaphore_signal(barrier, inc=1, device_id={"sp": partner(r)[1]}, device_id_type=MESH)
    pl.semaphore_signal(barrier, inc=1, device_id={"sp": lax.rem(sq + 1, n_sp)}, device_id_type=MESH)
    pl.semaphore_signal(barrier, inc=1, device_id={"sp": lax.rem(sq + n_sp - 1, n_sp)}, device_id_type=MESH)
    pl.semaphore_wait(barrier, n_tp - 1 + rounds + 2)

    def token_copy(k, c):
        return pltpu.make_async_remote_copy(
            src_ref=tok.at[pl.ds(c * ch, ch)],
            dst_ref=rows.at[pl.ds(pl.multiple_of(me * own + c * ch, 8), ch)],
            send_sem=tsend.at[k - 1, c],
            recv_sem=trecv.at[n_tp - k - 1, c],
            device_id={"tp": lax.rem(me + k, n_tp)},
            device_id_type=MESH,
        )

    sends = [token_copy(k, c) for c in range(nch) for k in range(1, n_tp)]
    for copy in sends:
        copy.start()
    rows[pl.ds(pl.multiple_of(me * own, 8), own), :] = tok[...]
    for load in loads:
        load.wait()
    gates[...] = jnp.zeros_like(gates)
    own_t[...] = jnp.zeros_like(own_t)

    def project(step, carry):
        k = step // nch
        c = step % nch
        owner = lax.rem(me + k, n_tp)
        r0 = pl.multiple_of(owner * own + c * ch, 8)
        spot = pl.ds(r0, ch)

        @pl.when(step >= nch)
        def _():
            pltpu.make_async_remote_copy(
                src_ref=tok.at[pl.ds(0, ch)],
                dst_ref=rows.at[spot],
                send_sem=tsend.at[0, 0],
                recv_sem=trecv.at[k - 1, c],
                device_id={"tp": owner},
                device_id_type=MESH,
            ).wait_recv()

        wide = rows[spot, :].astype(F32)
        scale = lax.rsqrt(jnp.mean(wide * wide, axis=1, keepdims=True) + EPS)
        normed = (wide * scale * gain[...].astype(F32)).astype(BF)

        def dot(w):
            return jnp.dot(normed, w[...], preferred_element_type=F32)

        gates[spot, 0:mh] = dot(gfo) + bfo[...]
        gates[spot, mh : 2 * mh] = dot(gin) + bin_[...]
        gates[spot, 2 * mh : 3 * mh] = extra[spot, :]
        gates[spot, 3 * mh : 4 * mh] = jnp.broadcast_to(p0[...], (ch, mh))
        aq[spot, :] = (dot(vq) * DQK ** -0.5).astype(BF)
        ak[spot, :] = dot(vk).astype(BF)
        av[spot, :] = dot(vv).astype(BF)
        ag[spot, :] = dot(vg).astype(BF)
        ao[spot, :] = dot(vo).astype(BF)
        inner = dot(vi).astype(BF).astype(F32)
        signal = dot(vs).astype(BF).astype(F32)
        mix[pl.ds(r0 + 8, ch), :] = inner * signal
        return carry

    lax.fori_loop(0, n_tp * nch, project, 0)
    for copy in sends:
        copy.wait_send()

    halo_send[...] = mix[total : total + 8, :]
    halo_copy = pltpu.make_async_remote_copy(
        src_ref=halo_send,
        dst_ref=mix.at[pl.ds(0, 8)],
        send_sem=hsem.at[0],
        recv_sem=hsem.at[1],
        device_id={"sp": lax.rem(sq + 1, n_sp)},
        device_id_type=MESH,
    )
    halo_copy.start()

    gates_t[...] = gates[...].T

    def own_rows(group):
        picked = [gates_t[pl.ds(group * mh + me * heads + h, 1), :] for h in range(heads)]
        picked += [jnp.zeros((8 - heads, total), F32)] if heads < 8 else []
        return jnp.concatenate(picked, axis=0)

    pre = own_rows(0)
    log_sig = jnp.minimum(pre, 0.0) - jnp.log1p(jnp.exp(-jnp.abs(pre)))
    log_forget = pos[...] * log_sig + own_rows(2)
    cumul = scan_lanes(log_forget, jnp.add, 0.0)
    lifted_in = own_rows(1) - cumul
    running = scan_lanes(lifted_in, jnp.maximum, FLOOR_LOG)
    own_t[0:8, :] = lifted_in
    own_t[8:16, :] = running
    own_c[...] = own_t[...].T
    last_peak = jnp.broadcast_to(running[:, total - 1 : total], (8, DV))
    last_decay = jnp.broadcast_to(cumul[:, total - 1 : total], (8, DV))

    states = []
    for h in range(heads):
        weight = jnp.exp(own_c[:, h : h + 1] - last_peak[h : h + 1, 0:1])
        keyed = (ak[:, h * DQK : (h + 1) * DQK].astype(F32) * weight).astype(BF)
        states.append(
            lax.dot_general(keyed, av[:, h * DV : (h + 1) * DV], (((0,), (0,)), ((), ())), preferred_element_type=F32)
        )
    mine = (states, last_decay + last_peak, last_decay)
    before = (
        [jnp.zeros((DQK, DV), F32) for _ in range(heads)],
        jnp.full((8, DV), FLOOR_LOG, F32),
        jnp.zeros((8, DV), F32),
    )

    tile = 256

    def local_part(h):
        qh = aq[:, h * DQK : (h + 1) * DQK]
        kh = ak[:, h * DQK : (h + 1) * DQK]
        for t in range(total // tile):
            lo, end = t * tile, (t + 1) * tile
            scores = lax.dot_general(
                qh[lo:end], kh[:end], (((1,), (1,)), ((), ())), preferred_element_type=F32
            )
            gap = own_t[h : h + 1, 0:end] - own_c[lo:end, 8 + h : 9 + h]
            row = lax.broadcasted_iota(jnp.int32, (tile, end), 0) + lo
            col = lax.broadcasted_iota(jnp.int32, (tile, end), 1)
            weighted = (scores * jnp.exp(jnp.where(col <= row, gap, FLOOR_LOG))).astype(BF)
            local[lo:end, h * DV : (h + 1) * DV] = jnp.dot(
                weighted, av[0:end, h * DV : (h + 1) * DV], preferred_element_type=F32
            )

    done = 0
    for r in range(rounds):
        bit, other = partner(r)
        for h in range(heads):
            st_send[r, h] = mine[0][h].astype(BF)
        sc_send[r, 0:8] = mine[1]
        sc_send[r, 8:16] = mine[2]
        copies = [
            pltpu.make_async_remote_copy(
                src_ref=src.at[r], dst_ref=dst.at[r], send_sem=ssend.at[r, i], recv_sem=srecv.at[r, i],
                device_id={"sp": other}, device_id_type=MESH,
            )
            for i, (src, dst) in enumerate(((st_send, st_recv), (sc_send, sc_recv)))
        ]
        for copy in copies:
            copy.start()
        want = heads if r == rounds - 1 else -(-heads * (r + 1) // rounds)
        while done < want:
            local_part(done)
            done += 1
        for copy in copies:
            copy.wait()
        theirs = ([st_recv[r, h].astype(F32) for h in range(heads)], sc_recv[r, 0:8], sc_recv[r, 8:16])
        later = bit == 1

        def pick(a, b):
            return ([jnp.where(later, x, y) for x, y in zip(a[0], b[0])], jnp.where(later, a[1], b[1]), jnp.where(later, a[2], b[2]))

        before = pick(merge(theirs, before), before)
        if r < rounds - 1:
            mine = merge(pick(theirs, mine), pick(mine, theirs))

    first = (
        [s0[me * heads + h] for h in range(heads)],
        own_rows(3)[:, 0:DV],
        jnp.zeros((8, DV), F32),
    )
    start = merge(first, before)
    for h in range(heads):
        start_s[h] = start[0][h].astype(BF)
    start_p[...] = start[1]
    halo_copy.wait()

    @pl.when(sq == 0)
    def _():
        mix[0:8, :] = jnp.zeros((8, cw), F32)

    taps_own = taps[:, pl.ds(pl.multiple_of(me * cw, 128), cw)].astype(F32)
    hg_own = hgain[:, pl.ds(pl.multiple_of(me * heads * DV, 128), heads * DV)].astype(F32)
    reach = taps.shape[0] - 1
    width = out.shape[1]
    piece = 512

    def finish(r0, dst, d0):
        spot = pl.ds(r0, ch)
        window = mix[pl.ds(r0, ch + 8), :]
        summed = jnp.zeros((ch, cw), F32)
        for j in range(reach + 1):
            at = 8 - reach + j
            summed = summed + taps_own[j : j + 1] * window[at : at + ch]
        conv = (ao[spot, :].astype(F32) * summed).astype(BF)
        cells = []
        for h in range(heads):
            side = slice(h * DV, (h + 1) * DV)
            top = own_c[spot, 8 + h : 9 + h]
            lead = start_p[h : h + 1, 0:1]
            peak = jnp.maximum(top, lead)
            remote = jnp.dot(aq[spot, h * DQK : (h + 1) * DQK], start_s[h], preferred_element_type=F32)
            num = jnp.exp(lead - peak) * remote + jnp.exp(top - peak) * local[spot, side]
            num = num * lax.rsqrt(jnp.mean(num * num, axis=1, keepdims=True) + EPS)
            cells.append((num * hg_own[:, side] * jax.nn.sigmoid(ag[spot, side].astype(F32))).astype(BF))
        memory = jnp.concatenate(cells, axis=1)
        for w0 in range(0, width, piece):
            cols = slice(w0, w0 + piece)
            term = jnp.dot(conv, vco[:, cols], preferred_element_type=F32) + jnp.dot(
                memory, vmo[:, cols], preferred_element_type=F32
            )
            dst[pl.ds(d0, ch), cols] = term.astype(BF)

    def part_copy(k, c):
        spot = pl.ds(pl.multiple_of((k - 1) * own + c * ch, 8), ch)
        back = pl.ds(pl.multiple_of((n_tp - k - 1) * own + c * ch, 8), ch)
        return pltpu.make_async_remote_copy(
            src_ref=part_send.at[spot],
            dst_ref=part_recv.at[back],
            send_sem=psend.at[k - 1, c],
            recv_sem=precv.at[n_tp - k - 1, c],
            device_id={"tp": lax.rem(me + k, n_tp)},
            device_id_type=MESH,
        )

    def for_peer(step, carry):
        k = step // nch + 1
        c = step % nch
        owner = lax.rem(me + k, n_tp)
        finish(
            pl.multiple_of(owner * own + c * ch, 8), part_send, pl.multiple_of((k - 1) * own + c * ch, 8)
        )
        part_copy(k, c).start()
        return carry

    lax.fori_loop(0, (n_tp - 1) * nch, for_peer, 0)

    def for_self(c, carry):
        finish(pl.multiple_of(me * own + c * ch, 8), out, pl.multiple_of(c * ch, 8))
        return carry

    lax.fori_loop(0, nch, for_self, 0)

    def gather_parts(c, carry):
        spot = pl.ds(pl.multiple_of(c * ch, 8), ch)
        acc = out[spot, :].astype(F32)
        for k in range(1, n_tp):
            part_copy(k, c).wait_send()
            pltpu.make_async_remote_copy(
                src_ref=part_send.at[pl.ds(0, ch)],
                dst_ref=part_recv.at[pl.ds(pl.multiple_of((k - 1) * own + c * ch, 8), ch)],
                send_sem=psend.at[0, 0],
                recv_sem=precv.at[k - 1, c],
                device_id={"tp": lax.rem(me + k, n_tp)},
                device_id_type=MESH,
            ).wait_recv()
            acc = acc + part_recv[pl.ds(pl.multiple_of((k - 1) * own + c * ch, 8), ch), :].astype(F32)
        out[spot, :] = acc.astype(BF)
        return carry

    lax.fori_loop(0, nch, gather_parts, 0)


def on_device(n_sp, n_tp, *args):
    (tok, gain, wo, wi, ws, taps, wq, wk, wv, wg, gin, gfo, bin_, bfo, pos, extra, s0, p0, hgain, wco, wmo) = args
    own, width = tok.shape
    total = own * n_tp
    cw = wo.shape[1]
    qw = wq.shape[1]
    vw = wv.shape[1]
    heads = qw // DQK
    ch = 128 if own % 128 == 0 else own
    nch = own // ch
    rounds = n_sp.bit_length() - 1
    vm = pl.BlockSpec(memory_space=pltpu.VMEM)
    hbm = pl.BlockSpec(memory_space=pl.ANY)
    weights = (2, 3, 4, 6, 7, 8, 9, 19, 20)
    V = pltpu.VMEM
    sem = pltpu.SemaphoreType.DMA
    return pl.pallas_call(
        functools.partial(kernel, n_sp, n_tp),
        out_shape=jax.ShapeDtypeStruct((own, width), BF),
        in_specs=[hbm if i in weights else vm for i in range(21)],
        out_specs=vm,
        scratch_shapes=[
            V((total, width), BF),
            V(wo.shape, BF), V(wi.shape, BF), V(ws.shape, BF), V(wq.shape, BF), V(wk.shape, BF),
            V(wv.shape, BF), V(wg.shape, BF), V(wco.shape, BF), V(wmo.shape, BF),
            V((total, cw), BF), V((total + 8, cw), F32), V((total, qw), BF), V((total, qw), BF),
            V((total, vw), BF), V((total, vw), BF), V((total, 128), F32), V((128, total), F32),
            V((128, total), F32), V((total, 128), F32), V((total, vw), F32), V((8, cw), F32),
            V((rounds, heads, DQK, DV), BF), V((rounds, heads, DQK, DV), BF),
            V((rounds, 16, DV), F32), V((rounds, 16, DV), F32),
            V((heads, DQK, DV), BF), V((8, DV), F32),
            V(((n_tp - 1) * own, width), BF), V(((n_tp - 1) * own, width), BF),
            sem((9,)), sem((n_tp - 1, nch)), sem((n_tp - 1, nch)), sem((2,)),
            sem((rounds, 2)), sem((rounds, 2)), sem((n_tp - 1, nch)), sem((n_tp - 1, nch)),
        ],
        compiler_params=pltpu.CompilerParams(
            collective_id=0, has_side_effects=True, vmem_limit_bytes=62 * 1024 * 1024
        ),
    )(
        tok, gain[None], wo, wi, ws, taps, wq, wk, wv, wg, gin, gfo, bin_[None], bfo[None],
        pos[None], extra, s0, p0[None], hgain[None], wco, wmo,
    )


def solution(mesh):
    cols = P(None, "tp")
    in_specs = (
        P(("sp", "tp"), None), P(), cols, cols, cols, P(), cols, cols, cols, cols, P(), P(), P(), P(),
        P("sp"), P("sp", None), P(), P(), P(), P("tp", None), P("tp", None),
    )
    body = functools.partial(on_device, mesh.shape["sp"], mesh.shape["tp"])
    return jax.shard_map(
        body, mesh=mesh, in_specs=in_specs, out_specs=P(("sp", "tp"), None), check_vma=False
    )
```

```python
import functools

import jax
import jax.numpy as jnp
from jax import lax
from jax.experimental import pallas as pl
from jax.experimental.pallas import tpu as pltpu
from jax.sharding import PartitionSpec as P

DQK = 64
DV = 128
EPS = 1e-06
FLOOR_LOG = -1e30
MESH = pl.DeviceIdType.MESH
BF = jnp.bfloat16
F32 = jnp.float32


def scan_lanes(x, op, fill):
    width = x.shape[1]
    lane = lax.broadcasted_iota(jnp.int32, x.shape, 1)
    shift = 1
    while shift < width:
        x = op(x, jnp.where(lane >= shift, pltpu.roll(x, shift, 1), fill))
        shift *= 2
    return x


def exchanges_middle(n_sp, n_tp, own, depth):
    return n_tp == 2 and n_sp % 4 == 0 and n_sp >= 8 and depth % (16 * n_sp) == 0 and own % 128 == 0


def merge(earlier, later):
    s1, p1, d1 = earlier
    s2, p2, d2 = later
    lifted = p1 + d2
    top = jnp.maximum(lifted, p2)
    w1 = jnp.exp(lifted - top)
    w2 = jnp.exp(p2 - top)
    return ([w1[h : h + 1] * s1[h] + w2[h : h + 1] * s2[h] for h in range(len(s1))], top, d1 + d2)


def kernel(
    n_sp, n_tp,
    tok, gain, wo, wi, ws, taps, wq, wk, wv, wg, gin, gfo, bin_, bfo, pos, extra, s0, p0, hgain, wco, wmo,
    out,
    rows, vo, vi, vs, vq, vk, vv, vg, vown, vother,
    ao, mix, aq, ak, av, ag, gates, gates_t, own_t, own_c, local, halo_send,
    st_send, st_recv, sc_send, sc_recv, start_s, start_p, part_send, part_recv,
    conv_own, conv_send, conv_recv, mem_own, mem_send, mem_recv, acc,
    wsem, tsend, trecv, hsem, ssend, srecv, psend, precv,
    xsem, zsend, zrecv, ysend, yrecv, csend, crecv, cvsend, cvrecv,
):
    me = lax.axis_index("tp")
    sq = lax.axis_index("sp")
    own = tok.shape[0]
    total = rows.shape[0]
    ch = 128 if own % 128 == 0 else own
    nch = own // ch
    heads = aq.shape[1] // DQK
    mh = gin.shape[0]
    cw = ao.shape[1]
    vw = av.shape[1]
    rounds = n_sp.bit_length() - 1
    middle = exchanges_middle(n_sp, n_tp, own, cw + vw)
    far = n_sp // 4
    bit_rows = (cw + vw) // n_sp
    vco, vmo = vown.at[0:cw], vown.at[cw : cw + vw]

    pairs = [(wco, vco), (wmo, vmo), (wo, vo), (wi, vi), (ws, vs), (wq, vq), (wk, vk), (wv, vv), (wg, vg)]
    loads = [pltpu.make_async_copy(src, dst, wsem.at[i]) for i, (src, dst) in enumerate(pairs)]
    for load in loads:
        load.start()

    def partner(r):
        bit = (sq // (1 << r)) % 2
        return bit, sq + (1 - 2 * bit) * (1 << r)

    barrier = pltpu.get_barrier_semaphore()
    for k in range(1, n_tp):
        pl.semaphore_signal(barrier, inc=1, device_id={"tp": lax.rem(me + k, n_tp)}, device_id_type=MESH)
    for r in range(rounds):
        pl.semaphore_signal(barrier, inc=1, device_id={"sp": partner(r)[1]}, device_id_type=MESH)
    pl.semaphore_signal(barrier, inc=1, device_id={"sp": lax.rem(sq + 1, n_sp)}, device_id_type=MESH)
    pl.semaphore_signal(barrier, inc=1, device_id={"sp": lax.rem(sq + n_sp - 1, n_sp)}, device_id_type=MESH)
    greeted = n_tp - 1 + rounds + 2
    if middle:
        for k in range(1, far):
            there = lax.rem(sq // 4 + k, far) * 4 + sq % 4
            pl.semaphore_signal(barrier, inc=1, device_id={"sp": there}, device_id_type=MESH)
        greeted += far - 1
    pl.semaphore_wait(barrier, greeted)

    def piece_of(index):
        return pl.ds(pl.multiple_of(index * bit_rows, 16), bit_rows)

    def relay(index, send, recv, device):
        return pltpu.make_async_remote_copy(
            src_ref=vother.at[piece_of(index)],
            dst_ref=vother.at[piece_of(index)],
            send_sem=send,
            recv_sem=recv,
            device_id=device,
            device_id_type=MESH,
        )

    flip_y, flip_c = partner(1)[1], partner(0)[1]

    def z_index(k):
        return lax.rem(sq // 4 + k, far) * 4 + sq % 4

    def z_send(k):
        return relay(sq, zsend.at[k - 1], zrecv.at[far - k - 1], {"sp": z_index(k)})

    def z_arrive(k):
        return relay(z_index(k), zsend.at[k - 1], zrecv.at[k - 1], {"sp": z_index(k)})

    def y_send(k):
        return relay(z_index(k), ysend.at[k], yrecv.at[k], {"sp": flip_y})

    def y_arrive(k):
        return relay(lax.rem(sq // 4 + k, far) * 4 + flip_y % 4, ysend.at[k], yrecv.at[k], {"sp": flip_y})

    def c_send(k):
        index = z_index(k) if k < far else lax.rem(sq // 4 + k - far, far) * 4 + flip_y % 4
        return relay(index, csend.at[k], crecv.at[k], {"sp": flip_c})

    def c_arrive(k):
        low = flip_c % 4 if k < far else 3 - sq % 4
        index = lax.rem(sq // 4 + k % far, far) * 4 + low
        return relay(index, csend.at[k], crecv.at[k], {"sp": flip_c})

    if middle:
        loads[0].wait()
        loads[1].wait()
        cross = pltpu.make_async_remote_copy(
            src_ref=vown.at[piece_of(sq)],
            dst_ref=vother.at[piece_of(sq)],
            send_sem=xsem.at[0],
            recv_sem=xsem.at[1],
            device_id={"tp": 1 - me},
            device_id_type=MESH,
        )
        cross.start()

    def token_copy(k, c):
        return pltpu.make_async_remote_copy(
            src_ref=tok.at[pl.ds(c * ch, ch)],
            dst_ref=rows.at[pl.ds(pl.multiple_of(me * own + c * ch, 8), ch)],
            send_sem=tsend.at[k - 1, c],
            recv_sem=trecv.at[n_tp - k - 1, c],
            device_id={"tp": lax.rem(me + k, n_tp)},
            device_id_type=MESH,
        )

    sends = [token_copy(k, c) for c in range(nch) for k in range(1, n_tp)]
    for copy in sends:
        copy.start()
    rows[pl.ds(pl.multiple_of(me * own, 8), own), :] = tok[...]
    for load in loads[2 if middle else 0 :]:
        load.wait()
    gates[...] = jnp.zeros_like(gates)
    own_t[...] = jnp.zeros_like(own_t)

    def project(step, carry):
        k = step // nch
        c = step % nch
        owner = lax.rem(me + k, n_tp)
        r0 = pl.multiple_of(owner * own + c * ch, 8)
        spot = pl.ds(r0, ch)

        if middle:

            @pl.when(step == nch)
            def _():
                cross.wait_recv()
                for j in range(1, far):
                    z_send(j).start()
                y_send(0).start()

            @pl.when(step == 2 * nch - 1)
            def _():
                for j in range(1, far):
                    z_arrive(j).wait_recv()
                    y_send(j).start()
                for j in range(far):
                    c_send(j).start()

        @pl.when(step >= nch)
        def _():
            pltpu.make_async_remote_copy(
                src_ref=tok.at[pl.ds(0, ch)],
                dst_ref=rows.at[spot],
                send_sem=tsend.at[0, 0],
                recv_sem=trecv.at[k - 1, c],
                device_id={"tp": owner},
                device_id_type=MESH,
            ).wait_recv()

        wide = rows[spot, :].astype(F32)
        scale = lax.rsqrt(jnp.mean(wide * wide, axis=1, keepdims=True) + EPS)
        normed = (wide * scale * gain[...].astype(F32)).astype(BF)

        def dot(w):
            return jnp.dot(normed, w[...], preferred_element_type=F32)

        def dot_t(w):
            return lax.dot_general(normed, w[...], (((1,), (1,)), ((), ())), preferred_element_type=F32)

        gates[spot, 0:mh] = dot_t(gfo) + bfo[...]
        gates[spot, mh : 2 * mh] = dot_t(gin) + bin_[...]
        gates[spot, 2 * mh : 3 * mh] = jnp.broadcast_to(p0[...], (ch, mh))
        aq[spot, :] = (dot(vq) * DQK ** -0.5).astype(BF)
        ak[spot, :] = dot(vk).astype(BF)
        av[spot, :] = dot(vv).astype(BF)
        ag[spot, :] = dot(vg).astype(BF)
        ao[spot, :] = dot(vo).astype(BF)
        inner = dot(vi).astype(BF).astype(F32)
        signal = dot(vs).astype(BF).astype(F32)
        mix[pl.ds(r0 + 8, ch), :] = inner * signal
        return carry

    lax.fori_loop(0, n_tp * nch, project, 0)
    for copy in sends:
        copy.wait_send()

    halo_send[...] = mix[total : total + 8, :]
    halo_copy = pltpu.make_async_remote_copy(
        src_ref=halo_send,
        dst_ref=mix.at[pl.ds(0, 8)],
        send_sem=hsem.at[0],
        recv_sem=hsem.at[1],
        device_id={"sp": lax.rem(sq + 1, n_sp)},
        device_id_type=MESH,
    )
    halo_copy.start()

    gates_t[...] = gates[...].T

    def own_rows(group, source=gates_t):
        picked = [source[pl.ds(group * mh + me * heads + h, 1), :] for h in range(heads)]
        picked += [jnp.zeros((8 - heads, total), F32)] if heads < 8 else []
        return jnp.concatenate(picked, axis=0)

    pre = own_rows(0)
    log_sig = jnp.minimum(pre, 0.0) - jnp.log1p(jnp.exp(-jnp.abs(pre)))
    log_forget = pos[...] * log_sig + own_rows(0, extra)
    cumul = scan_lanes(log_forget, jnp.add, 0.0)
    lifted_in = own_rows(1) - cumul
    running = scan_lanes(lifted_in, jnp.maximum, FLOOR_LOG)
    own_t[0:8, :] = lifted_in
    own_t[8:16, :] = running
    own_c[...] = own_t[...].T
    last_peak = jnp.broadcast_to(running[:, total - 1 : total], (8, DV))
    last_decay = jnp.broadcast_to(cumul[:, total - 1 : total], (8, DV))

    states = []
    for h in range(heads):
        weight = jnp.exp(own_c[:, h : h + 1] - last_peak[h : h + 1, 0:1])
        keyed = (ak[:, h * DQK : (h + 1) * DQK].astype(F32) * weight).astype(BF)
        states.append(
            lax.dot_general(keyed, av[:, h * DV : (h + 1) * DV], (((0,), (0,)), ((), ())), preferred_element_type=F32)
        )
    mine = (states, last_decay + last_peak, last_decay)
    before = (
        [jnp.zeros((DQK, DV), F32) for _ in range(heads)],
        jnp.full((8, DV), FLOOR_LOG, F32),
        jnp.zeros((8, DV), F32),
    )

    tile = 256

    def local_part(h):
        qh = aq[:, h * DQK : (h + 1) * DQK]
        kh = ak[:, h * DQK : (h + 1) * DQK]
        for t in range(total // tile):
            lo, end = t * tile, (t + 1) * tile
            scores = lax.dot_general(
                qh[lo:end], kh[:end], (((1,), (1,)), ((), ())), preferred_element_type=F32
            )
            gap = own_t[h : h + 1, 0:end] - own_c[lo:end, 8 + h : 9 + h]
            row = lax.broadcasted_iota(jnp.int32, (tile, end), 0) + lo
            col = lax.broadcasted_iota(jnp.int32, (tile, end), 1)
            weighted = (scores * jnp.exp(jnp.where(col <= row, gap, FLOOR_LOG))).astype(BF)
            local[lo:end, h * DV : (h + 1) * DV] = jnp.dot(
                weighted, av[0:end, h * DV : (h + 1) * DV], preferred_element_type=F32
            )

    taps_own = taps[:, pl.ds(pl.multiple_of(me * cw, 128), cw)].astype(F32)
    hg_own = hgain[:, pl.ds(pl.multiple_of(me * heads * DV, 128), heads * DV)].astype(F32)
    reach = taps.shape[0] - 1

    def conv_rows(r0):
        window = mix[pl.ds(r0, ch + 8), :]
        summed = jnp.zeros((ch, cw), F32)
        for j in range(reach + 1):
            at = 8 - reach + j
            summed = summed + taps_own[j : j + 1] * window[at : at + ch]
        return (ao[pl.ds(r0, ch), :].astype(F32) * summed).astype(BF)

    def mid_copy(src, dst, send, recv, c):
        rows_c = pl.ds(pl.multiple_of(c * ch, 8), ch)
        return pltpu.make_async_remote_copy(
            src_ref=src.at[rows_c], dst_ref=dst.at[rows_c], send_sem=send, recv_sem=recv,
            device_id={"tp": 1 - me}, device_id_type=MESH,
        )

    def conv_all():
        def one(c, carry):
            rows_c = pl.ds(pl.multiple_of(c * ch, 8), ch)
            conv_send[rows_c, :] = conv_rows(pl.multiple_of((1 - me) * own + c * ch, 8))
            mid_copy(conv_send, conv_recv, cvsend.at[c], cvrecv.at[c], c).start()
            return carry

        def two(c, carry):
            conv_own[pl.ds(pl.multiple_of(c * ch, 8), ch), :] = conv_rows(pl.multiple_of(me * own + c * ch, 8))
            return carry

        lax.fori_loop(0, nch, one, 0)
        lax.fori_loop(0, nch, two, 0)

    done = 0
    for r in range(rounds):
        bit, other = partner(r)
        for h in range(heads):
            st_send[r, h] = mine[0][h].astype(BF)
        sc_send[r, 0:8] = mine[1]
        sc_send[r, 8:16] = mine[2]
        copies = [
            pltpu.make_async_remote_copy(
                src_ref=src.at[r], dst_ref=dst.at[r], send_sem=ssend.at[r, i], recv_sem=srecv.at[r, i],
                device_id={"sp": other}, device_id_type=MESH,
            )
            for i, (src, dst) in enumerate(((st_send, st_recv), (sc_send, sc_recv)))
        ]
        for copy in copies:
            copy.start()
        if r == 0:
            halo_copy.wait()

            @pl.when(sq == 0)
            def _():
                mix[0:8, :] = jnp.zeros((8, cw), F32)

            if middle:
                conv_all()
        want = heads if r == rounds - 1 else -(-heads * (r + 1) // rounds)
        while done < want:
            local_part(done)
            done += 1
        if middle and r == rounds - 1:
            for k in range(far):
                y_arrive(k).wait_recv()
                c_send(far + k).start()
        for copy in copies:
            copy.wait()
        theirs = ([st_recv[r, h].astype(F32) for h in range(heads)], sc_recv[r, 0:8], sc_recv[r, 8:16])
        later = bit == 1

        def pick(a, b):
            return ([jnp.where(later, x, y) for x, y in zip(a[0], b[0])], jnp.where(later, a[1], b[1]), jnp.where(later, a[2], b[2]))

        before = pick(merge(theirs, before), before)
        if r < rounds - 1:
            mine = merge(pick(theirs, mine), pick(mine, theirs))

    first = (
        [s0[me * heads + h] for h in range(heads)],
        own_rows(2)[:, 0:DV],
        jnp.zeros((8, DV), F32),
    )
    start = merge(first, before)
    for h in range(heads):
        start_s[h] = start[0][h].astype(BF)
    start_p[...] = start[1]
    width = out.shape[1]
    piece = 512

    def finish(r0, dst, d0):
        conv = conv_rows(r0)
        memory = memory_rows(r0)
        for w0 in range(0, width, piece):
            cols = slice(w0, w0 + piece)
            term = jnp.dot(conv, vown[0:cw, cols], preferred_element_type=F32) + jnp.dot(
                memory, vown[cw : cw + vw, cols], preferred_element_type=F32
            )
            dst[pl.ds(d0, ch), cols] = term.astype(BF)

    def memory_rows(r0):
        spot = pl.ds(r0, ch)
        cells = []
        for h in range(heads):
            side = slice(h * DV, (h + 1) * DV)
            top = own_c[spot, 8 + h : 9 + h]
            lead = start_p[h : h + 1, 0:1]
            peak = jnp.maximum(top, lead)
            remote = jnp.dot(aq[spot, h * DQK : (h + 1) * DQK], start_s[h], preferred_element_type=F32)
            num = jnp.exp(lead - peak) * remote + jnp.exp(top - peak) * local[spot, side]
            num = num * lax.rsqrt(jnp.mean(num * num, axis=1, keepdims=True) + EPS)
            cells.append((num * hg_own[:, side] * jax.nn.sigmoid(ag[spot, side].astype(F32))).astype(BF))
        return jnp.concatenate(cells, axis=1)

    if middle:
        peer0, own0 = (1 - me) * own, me * own

        def memory_peer(c, carry):
            rows_c = pl.ds(pl.multiple_of(c * ch, 8), ch)
            mem_send[rows_c, :] = memory_rows(pl.multiple_of(peer0 + c * ch, 8))
            mid_copy(mem_send, mem_recv, psend.at[0, c], precv.at[0, c], c).start()
            return carry

        lax.fori_loop(0, nch, memory_peer, 0)
        for k in range(2 * far):
            c_arrive(k).wait_recv()

        def own_terms(c, carry):
            rows_c = pl.ds(pl.multiple_of(c * ch, 8), ch)
            conv = conv_own[rows_c, :]
            mid_copy(conv_send, conv_recv, cvsend.at[c], cvrecv.at[c], c).wait()
            other = conv_recv[rows_c, :]
            memory = memory_rows(pl.multiple_of(own0 + c * ch, 8))
            for w0 in range(0, width, piece):
                cols = slice(w0, w0 + piece)
                acc[rows_c, cols] = (
                    jnp.dot(conv, vown[0:cw, cols], preferred_element_type=F32)
                    + jnp.dot(other, vother[0:cw, cols], preferred_element_type=F32)
                    + jnp.dot(memory, vown[cw : cw + vw, cols], preferred_element_type=F32)
                )
            return carry

        lax.fori_loop(0, nch, own_terms, 0)

        def last_terms(c, carry):
            rows_c = pl.ds(pl.multiple_of(c * ch, 8), ch)
            mid_copy(mem_send, mem_recv, psend.at[0, c], precv.at[0, c], c).wait()
            memory = mem_recv[rows_c, :]
            for w0 in range(0, width, piece):
                cols = slice(w0, w0 + piece)
                out[rows_c, cols] = (
                    acc[rows_c, cols]
                    + jnp.dot(memory, vother[cw : cw + vw, cols], preferred_element_type=F32)
                ).astype(BF)
            return carry

        lax.fori_loop(0, nch, last_terms, 0)
        cross.wait_send()
        for k in range(1, far):
            z_send(k).wait_send()
        for k in range(far):
            y_send(k).wait_send()
        for k in range(2 * far):
            c_send(k).wait_send()
        return

    def part_copy(k, c):
        spot = pl.ds(pl.multiple_of((k - 1) * own + c * ch, 8), ch)
        back = pl.ds(pl.multiple_of((n_tp - k - 1) * own + c * ch, 8), ch)
        return pltpu.make_async_remote_copy(
            src_ref=part_send.at[spot],
            dst_ref=part_recv.at[back],
            send_sem=psend.at[k - 1, c],
            recv_sem=precv.at[n_tp - k - 1, c],
            device_id={"tp": lax.rem(me + k, n_tp)},
            device_id_type=MESH,
        )

    def for_peer(step, carry):
        k = step // nch + 1
        c = step % nch
        owner = lax.rem(me + k, n_tp)
        finish(
            pl.multiple_of(owner * own + c * ch, 8), part_send, pl.multiple_of((k - 1) * own + c * ch, 8)
        )
        part_copy(k, c).start()
        return carry

    lax.fori_loop(0, (n_tp - 1) * nch, for_peer, 0)

    def for_self(c, carry):
        finish(pl.multiple_of(me * own + c * ch, 8), out, pl.multiple_of(c * ch, 8))
        return carry

    lax.fori_loop(0, nch, for_self, 0)

    def gather_parts(c, carry):
        spot = pl.ds(pl.multiple_of(c * ch, 8), ch)
        acc = out[spot, :].astype(F32)
        for k in range(1, n_tp):
            part_copy(k, c).wait_send()
            pltpu.make_async_remote_copy(
                src_ref=part_send.at[pl.ds(0, ch)],
                dst_ref=part_recv.at[pl.ds(pl.multiple_of((k - 1) * own + c * ch, 8), ch)],
                send_sem=psend.at[0, 0],
                recv_sem=precv.at[k - 1, c],
                device_id={"tp": lax.rem(me + k, n_tp)},
                device_id_type=MESH,
            ).wait_recv()
            acc = acc + part_recv[pl.ds(pl.multiple_of((k - 1) * own + c * ch, 8), ch), :].astype(F32)
        out[spot, :] = acc.astype(BF)
        return carry

    lax.fori_loop(0, nch, gather_parts, 0)


def on_device(n_sp, n_tp, *args):
    (tok, gain, wo, wi, ws, taps, wq, wk, wv, wg, gin, gfo, bin_, bfo, pos, extra, s0, p0, hgain, wco, wmo) = args
    own, width = tok.shape
    total = own * n_tp
    cw = wo.shape[1]
    qw = wq.shape[1]
    vw = wv.shape[1]
    heads = qw // DQK
    ch = 128 if own % 128 == 0 else own
    nch = own // ch
    rounds = n_sp.bit_length() - 1
    middle = exchanges_middle(n_sp, n_tp, own, cw + vw)
    far = max(n_sp // 4, 1)
    vm = pl.BlockSpec(memory_space=pltpu.VMEM)
    hbm = pl.BlockSpec(memory_space=pl.ANY)
    weights = (2, 3, 4, 6, 7, 8, 9, 19, 20)
    V = pltpu.VMEM
    sem = pltpu.SemaphoreType.DMA
    return pl.pallas_call(
        functools.partial(kernel, n_sp, n_tp),
        out_shape=jax.ShapeDtypeStruct((own, width), BF),
        in_specs=[hbm if i in weights else vm for i in range(21)],
        out_specs=vm,
        scratch_shapes=[
            V((total, width), BF),
            V(wo.shape, BF), V(wi.shape, BF), V(ws.shape, BF), V(wq.shape, BF), V(wk.shape, BF),
            V(wv.shape, BF), V(wg.shape, BF), V((cw + vw, width), BF), V((cw + vw if middle else 16, width), BF),
            V((total, cw), BF), V((total + 8, cw), F32), V((total, qw), BF), V((total, qw), BF),
            V((total, vw), BF), V((total, vw), BF), V((total, 128), F32), V((128, total), F32),
            V((128, total), F32), V((total, 128), F32), V((total, vw), F32), V((8, cw), F32),
            V((rounds, heads, DQK, DV), BF), V((rounds, heads, DQK, DV), BF),
            V((rounds, 16, DV), F32), V((rounds, 16, DV), F32),
            V((heads, DQK, DV), BF), V((8, DV), F32),
            V((16 if middle else (n_tp - 1) * own, width), BF), V((16 if middle else (n_tp - 1) * own, width), BF),
            *[V((own if middle else 16, cw), BF)] * 3, *[V((own if middle else 16, vw), BF)] * 3,
            V((own if middle else 8, width), F32),
            sem((9,)), sem((n_tp - 1, nch)), sem((n_tp - 1, nch)), sem((2,)),
            sem((rounds, 2)), sem((rounds, 2)), sem((n_tp - 1, nch)), sem((n_tp - 1, nch)),
            sem((2,)), sem((far,)), sem((far,)), sem((far,)), sem((far,)), sem((2 * far,)), sem((2 * far,)), sem((nch,)), sem((nch,)),
        ],
        compiler_params=pltpu.CompilerParams(
            collective_id=0, has_side_effects=True, vmem_limit_bytes=62 * 1024 * 1024
        ),
    )(
        tok, gain.reshape(1, -1), wo, wi, ws, taps, wq, wk, wv, wg, gin.T, gfo.T, bin_.reshape(1, -1),
        bfo.reshape(1, -1), pos.reshape(1, -1), extra.T, s0, p0.reshape(1, -1), hgain.reshape(1, -1), wco, wmo,
    )


def solution(mesh):
    cols = P(None, "tp")
    in_specs = (
        P(("sp", "tp"), None), P(), cols, cols, cols, P(), cols, cols, cols, cols, P(), P(), P(), P(),
        P("sp"), P("sp", None), P(), P(), P(), P("tp", None), P("tp", None),
    )
    body = functools.partial(on_device, mesh.shape["sp"], mesh.shape["tp"])
    return jax.shard_map(
        body, mesh=mesh, in_specs=in_specs, out_specs=P(("sp", "tp"), None), check_vma=False
    )
```

```python
import functools

import jax
import jax.numpy as jnp
from jax import lax
from jax.experimental import pallas as pl
from jax.experimental.pallas import tpu as pltpu
from jax.sharding import PartitionSpec as P

DQK = 64
DV = 128
EPS = 1e-06
FLOOR_LOG = -1e30
MESH = pl.DeviceIdType.MESH
BF = jnp.bfloat16
F32 = jnp.float32


def scan_lanes(x, op, fill):
    width = x.shape[1]
    lane = lax.broadcasted_iota(jnp.int32, x.shape, 1)
    shift = 1
    while shift < width:
        x = op(x, jnp.where(lane >= shift, pltpu.roll(x, shift, 1), fill))
        shift *= 2
    return x


def exchanges_middle(n_sp, n_tp, own, cw, depth):
    return n_tp == 2 and n_sp % 4 == 0 and n_sp >= 8 and cw % (depth // n_sp) == 0 and depth % (16 * n_sp) == 0 and own % 128 == 0


def flat(ref):
    rows = ref[...].astype(F32)
    return jnp.concatenate([rows[i : i + 1] for i in range(rows.shape[0])], axis=1)


def merge(earlier, later):
    s1, p1, d1 = earlier
    s2, p2, d2 = later
    lifted = p1 + d2
    top = jnp.maximum(lifted, p2)
    w1 = jnp.exp(lifted - top)
    w2 = jnp.exp(p2 - top)
    return ([w1[h : h + 1] * s1[h] + w2[h : h + 1] * s2[h] for h in range(len(s1))], top, d1 + d2)


def kernel(
    n_sp, n_tp,
    tok, gain, wo, wi, ws, taps, wq, wk, wv, wg, gin, gfo, bin_, bfo, pos, extra, s0, p0, hgain, wco, wmo,
    out,
    rows, vo, vi, vs, vq, vk, vv, vg, vown, vother,
    ao, mix, aq, ak, av, ag, gates, gates_t, own_t, own_c, local, halo_send,
    st_send, st_recv, sc_send, sc_recv, start_s, start_p, part_send, part_recv,
    gain_row, hg_rows, conv_own, conv_send, conv_recv, mem_own, mem_send, mem_recv, acc,
    wsem, tsend, trecv, hsem, ssend, srecv, psend, precv,
    xsem, zsend, zrecv, ysend, yrecv, csend, crecv, cvsend, cvrecv,
):
    me = lax.axis_index("tp")
    sq = lax.axis_index("sp")
    own = tok.shape[0]
    total = rows.shape[0]
    ch = 128 if own % 128 == 0 else own
    nch = own // ch
    heads = aq.shape[1] // DQK
    mh = gin.shape[0]
    cw = ao.shape[1]
    vw = av.shape[1]
    rounds = n_sp.bit_length() - 1
    middle = exchanges_middle(n_sp, n_tp, own, cw, cw + vw)
    far = n_sp // 4
    bit_rows = (cw + vw) // n_sp
    vco, vmo = vown.at[0:cw], vown.at[cw : cw + vw]

    pairs = [(wq, vq), (wk, vk), (wv, vv), (wg, vg), (wo, vo), (wi, vi), (ws, vs), (wco, vco), (wmo, vmo)]
    loads = [pltpu.make_async_copy(src, dst, wsem.at[i]) for i, (src, dst) in enumerate(pairs)]
    for load in loads:
        load.start()

    def partner(r):
        bit = (sq // (1 << r)) % 2
        return bit, sq + (1 - 2 * bit) * (1 << r)

    barrier = pltpu.get_barrier_semaphore()
    for k in range(1, n_tp):
        pl.semaphore_signal(barrier, inc=1, device_id={"tp": lax.rem(me + k, n_tp)}, device_id_type=MESH)
    for r in range(rounds):
        pl.semaphore_signal(barrier, inc=1, device_id={"sp": partner(r)[1]}, device_id_type=MESH)
    pl.semaphore_signal(barrier, inc=1, device_id={"sp": lax.rem(sq + 1, n_sp)}, device_id_type=MESH)
    pl.semaphore_signal(barrier, inc=1, device_id={"sp": lax.rem(sq + n_sp - 1, n_sp)}, device_id_type=MESH)
    greeted = n_tp - 1 + rounds + 2
    if middle:
        for k in range(1, far):
            there = lax.rem(sq // 4 + k, far) * 4 + sq % 4
            pl.semaphore_signal(barrier, inc=1, device_id={"sp": there}, device_id_type=MESH)
        greeted += far - 1
    pl.semaphore_wait(barrier, greeted)

    def piece_of(index):
        return pl.ds(pl.multiple_of(index * bit_rows, 16), bit_rows)

    def relay(index, send, recv, device):
        return pltpu.make_async_remote_copy(
            src_ref=vother.at[piece_of(index)],
            dst_ref=vother.at[piece_of(index)],
            send_sem=send,
            recv_sem=recv,
            device_id=device,
            device_id_type=MESH,
        )

    flip_y, flip_c = partner(1)[1], partner(0)[1]

    def z_index(k):
        return lax.rem(sq // 4 + k, far) * 4 + sq % 4

    def z_send(k):
        return relay(sq, zsend.at[k - 1], zrecv.at[far - k - 1], {"sp": z_index(k)})

    def z_arrive(k):
        return relay(z_index(k), zsend.at[k - 1], zrecv.at[k - 1], {"sp": z_index(k)})

    def y_send(k):
        return relay(z_index(k), ysend.at[k], yrecv.at[k], {"sp": flip_y})

    def y_arrive(k):
        return relay(lax.rem(sq // 4 + k, far) * 4 + flip_y % 4, ysend.at[k], yrecv.at[k], {"sp": flip_y})

    def c_send(k):
        index = z_index(k) if k < far else lax.rem(sq // 4 + k - far, far) * 4 + flip_y % 4
        return relay(index, csend.at[k], crecv.at[k], {"sp": flip_c})

    def c_arrive(k):
        low = flip_c % 4 if k < far else 3 - sq % 4
        index = lax.rem(sq // 4 + k % far, far) * 4 + low
        return relay(index, csend.at[k], crecv.at[k], {"sp": flip_c})

    def cross_copy(src, index):
        return pltpu.make_async_remote_copy(
            src_ref=src.at[piece_of(index)],
            dst_ref=vother.at[piece_of(sq)],
            send_sem=xsem.at[0],
            recv_sem=xsem.at[1],
            device_id={"tp": 1 - me},
            device_id_type=MESH,
        )

    if middle:
        cross = cross_copy(wco, 0)
        split = cw // bit_rows

        @pl.when(sq < split)
        def _():
            cross_copy(wco, sq).start()

        @pl.when(sq >= split)
        def _():
            cross_copy(wmo, sq - split).start()

    def token_copy(k, c):
        return pltpu.make_async_remote_copy(
            src_ref=tok.at[pl.ds(c * ch, ch)],
            dst_ref=rows.at[pl.ds(pl.multiple_of(me * own + c * ch, 8), ch)],
            send_sem=tsend.at[k - 1, c],
            recv_sem=trecv.at[n_tp - k - 1, c],
            device_id={"tp": lax.rem(me + k, n_tp)},
            device_id_type=MESH,
        )

    sends = [token_copy(k, c) for c in range(nch) for k in range(1, n_tp)]
    for copy in sends:
        copy.start()
    rows[pl.ds(pl.multiple_of(me * own, 8), own), :] = tok[...]
    for load in loads:
        load.wait()
    gain_row[...] = flat(gain)
    hg_rows[...] = hgain[...].astype(F32)
    gates[...] = jnp.zeros_like(gates)
    own_t[...] = jnp.zeros_like(own_t)

    def project(step, carry):
        k = step // nch
        c = step % nch
        owner = lax.rem(me + k, n_tp)
        r0 = pl.multiple_of(owner * own + c * ch, 8)
        spot = pl.ds(r0, ch)

        if middle:

            @pl.when(step == nch)
            def _():
                cross.wait_recv()
                for j in range(1, far):
                    z_send(j).start()
                y_send(0).start()

            @pl.when(step == 2 * nch - 1)
            def _():
                for j in range(1, far):
                    z_arrive(j).wait_recv()
                    y_send(j).start()
                for j in range(far):
                    c_send(j).start()

        @pl.when(step >= nch)
        def _():
            pltpu.make_async_remote_copy(
                src_ref=tok.at[pl.ds(0, ch)],
                dst_ref=rows.at[spot],
                send_sem=tsend.at[0, 0],
                recv_sem=trecv.at[k - 1, c],
                device_id={"tp": owner},
                device_id_type=MESH,
            ).wait_recv()

        wide = rows[spot, :].astype(F32)
        scale = lax.rsqrt(jnp.mean(wide * wide, axis=1, keepdims=True) + EPS)
        normed = (wide * scale * gain_row[...]).astype(BF)

        def dot(w):
            return jnp.dot(normed, w[...], preferred_element_type=F32)

        def dot_t(w):
            return lax.dot_general(normed, w[...], (((1,), (1,)), ((), ())), preferred_element_type=F32)

        gates[spot, 0:mh] = dot_t(gfo) + bfo[...]
        gates[spot, mh : 2 * mh] = dot_t(gin) + bin_[...]
        gates[spot, 2 * mh : 3 * mh] = jnp.broadcast_to(p0[...], (ch, mh))
        aq[spot, :] = (dot(vq) * DQK ** -0.5).astype(BF)
        ak[spot, :] = dot(vk).astype(BF)
        av[spot, :] = dot(vv).astype(BF)
        ag[spot, :] = dot(vg).astype(BF)
        ao[spot, :] = dot(vo).astype(BF)
        inner = dot(vi).astype(BF).astype(F32)
        signal = dot(vs).astype(BF).astype(F32)
        mix[pl.ds(r0 + 8, ch), :] = inner * signal
        return carry

    lax.fori_loop(0, n_tp * nch, project, 0)
    for copy in sends:
        copy.wait_send()

    halo_send[...] = mix[total : total + 8, :]
    halo_copy = pltpu.make_async_remote_copy(
        src_ref=halo_send,
        dst_ref=mix.at[pl.ds(0, 8)],
        send_sem=hsem.at[0],
        recv_sem=hsem.at[1],
        device_id={"sp": lax.rem(sq + 1, n_sp)},
        device_id_type=MESH,
    )
    halo_copy.start()

    gates_t[...] = gates[...].T

    def own_rows(group, source=gates_t):
        picked = [source[pl.ds(group * mh + me * heads + h, 1), :] for h in range(heads)]
        picked += [jnp.zeros((8 - heads, total), F32)] if heads < 8 else []
        return jnp.concatenate(picked, axis=0)

    pre = own_rows(0)
    log_sig = jnp.minimum(pre, 0.0) - jnp.log1p(jnp.exp(-jnp.abs(pre)))
    log_forget = flat(pos) * log_sig + own_rows(0, extra)
    cumul = scan_lanes(log_forget, jnp.add, 0.0)
    lifted_in = own_rows(1) - cumul
    running = scan_lanes(lifted_in, jnp.maximum, FLOOR_LOG)
    own_t[0:8, :] = lifted_in
    own_t[8:16, :] = running
    own_c[...] = own_t[...].T
    last_peak = jnp.broadcast_to(running[:, total - 1 : total], (8, DV))
    last_decay = jnp.broadcast_to(cumul[:, total - 1 : total], (8, DV))

    states = []
    for h in range(heads):
        weight = jnp.exp(own_c[:, h : h + 1] - last_peak[h : h + 1, 0:1])
        keyed = (ak[:, h * DQK : (h + 1) * DQK].astype(F32) * weight).astype(BF)
        states.append(
            lax.dot_general(keyed, av[:, h * DV : (h + 1) * DV], (((0,), (0,)), ((), ())), preferred_element_type=F32)
        )
    mine = (states, last_decay + last_peak, last_decay)
    before = (
        [jnp.zeros((DQK, DV), F32) for _ in range(heads)],
        jnp.full((8, DV), FLOOR_LOG, F32),
        jnp.zeros((8, DV), F32),
    )

    tile = 256

    def local_part(h):
        qh = aq[:, h * DQK : (h + 1) * DQK]
        kh = ak[:, h * DQK : (h + 1) * DQK]
        for t in range(total // tile):
            lo, end = t * tile, (t + 1) * tile
            scores = lax.dot_general(
                qh[lo:end], kh[:end], (((1,), (1,)), ((), ())), preferred_element_type=F32
            )
            gap = own_t[h : h + 1, 0:end] - own_c[lo:end, 8 + h : 9 + h]
            row = lax.broadcasted_iota(jnp.int32, (tile, end), 0) + lo
            col = lax.broadcasted_iota(jnp.int32, (tile, end), 1)
            weighted = (scores * jnp.exp(jnp.where(col <= row, gap, FLOOR_LOG))).astype(BF)
            local[lo:end, h * DV : (h + 1) * DV] = jnp.dot(
                weighted, av[0:end, h * DV : (h + 1) * DV], preferred_element_type=F32
            )

    taps_own = taps[:, pl.ds(pl.multiple_of(me * cw, 128), cw)].astype(F32)
    reach = taps.shape[0] - 1

    def conv_rows(r0):
        window = mix[pl.ds(r0, ch + 8), :]
        summed = jnp.zeros((ch, cw), F32)
        for j in range(reach + 1):
            at = 8 - reach + j
            summed = summed + taps_own[j : j + 1] * window[at : at + ch]
        return (ao[pl.ds(r0, ch), :].astype(F32) * summed).astype(BF)

    def mid_copy(src, dst, send, recv, c):
        rows_c = pl.ds(pl.multiple_of(c * ch, 8), ch)
        return pltpu.make_async_remote_copy(
            src_ref=src.at[rows_c], dst_ref=dst.at[rows_c], send_sem=send, recv_sem=recv,
            device_id={"tp": 1 - me}, device_id_type=MESH,
        )

    def conv_all():
        def one(c, carry):
            rows_c = pl.ds(pl.multiple_of(c * ch, 8), ch)
            conv_send[rows_c, :] = conv_rows(pl.multiple_of((1 - me) * own + c * ch, 8))
            mid_copy(conv_send, conv_recv, cvsend.at[c], cvrecv.at[c], c).start()
            return carry

        def two(c, carry):
            conv_own[pl.ds(pl.multiple_of(c * ch, 8), ch), :] = conv_rows(pl.multiple_of(me * own + c * ch, 8))
            return carry

        lax.fori_loop(0, nch, one, 0)
        lax.fori_loop(0, nch, two, 0)

    done = 0
    for r in range(rounds):
        bit, other = partner(r)
        for h in range(heads):
            st_send[r, h] = mine[0][h].astype(BF)
        sc_send[r, 0:8] = mine[1]
        sc_send[r, 8:16] = mine[2]
        copies = [
            pltpu.make_async_remote_copy(
                src_ref=src.at[r], dst_ref=dst.at[r], send_sem=ssend.at[r, i], recv_sem=srecv.at[r, i],
                device_id={"sp": other}, device_id_type=MESH,
            )
            for i, (src, dst) in enumerate(((st_send, st_recv), (sc_send, sc_recv)))
        ]
        for copy in copies:
            copy.start()
        if r == 0:
            halo_copy.wait()

            @pl.when(sq == 0)
            def _():
                mix[0:8, :] = jnp.zeros((8, cw), F32)

            if middle:
                conv_all()
        want = heads if r == rounds - 1 else -(-heads * (r + 1) // rounds)
        while done < want:
            local_part(done)
            done += 1
        if middle and r == rounds - 1:
            for k in range(far):
                y_arrive(k).wait_recv()
                c_send(far + k).start()
        for copy in copies:
            copy.wait()
        theirs = ([st_recv[r, h].astype(F32) for h in range(heads)], sc_recv[r, 0:8], sc_recv[r, 8:16])
        later = bit == 1

        def pick(a, b):
            return ([jnp.where(later, x, y) for x, y in zip(a[0], b[0])], jnp.where(later, a[1], b[1]), jnp.where(later, a[2], b[2]))

        before = pick(merge(theirs, before), before)
        if r < rounds - 1:
            mine = merge(pick(theirs, mine), pick(mine, theirs))

    first = (
        [s0[me * heads + h] for h in range(heads)],
        own_rows(2)[:, 0:DV],
        jnp.zeros((8, DV), F32),
    )
    start = merge(first, before)
    for h in range(heads):
        start_s[h] = start[0][h].astype(BF)
    start_p[...] = start[1]
    width = out.shape[1]
    piece = 512

    def finish(r0, dst, d0):
        conv = conv_rows(r0)
        memory = memory_rows(r0)
        for w0 in range(0, width, piece):
            cols = slice(w0, w0 + piece)
            term = jnp.dot(conv, vown[0:cw, cols], preferred_element_type=F32) + jnp.dot(
                memory, vown[cw : cw + vw, cols], preferred_element_type=F32
            )
            dst[pl.ds(d0, ch), cols] = term.astype(BF)

    def memory_rows(r0):
        spot = pl.ds(r0, ch)
        cells = []
        for h in range(heads):
            side = slice(h * DV, (h + 1) * DV)
            top = own_c[spot, 8 + h : 9 + h]
            lead = start_p[h : h + 1, 0:1]
            peak = jnp.maximum(top, lead)
            remote = jnp.dot(aq[spot, h * DQK : (h + 1) * DQK], start_s[h], preferred_element_type=F32)
            num = jnp.exp(lead - peak) * remote + jnp.exp(top - peak) * local[spot, side]
            num = num * lax.rsqrt(jnp.mean(num * num, axis=1, keepdims=True) + EPS)
            cells.append((num * hg_rows[pl.ds(me * heads + h, 1), :] * jax.nn.sigmoid(ag[spot, side].astype(F32))).astype(BF))
        return jnp.concatenate(cells, axis=1)

    if middle:
        peer0, own0 = (1 - me) * own, me * own

        def memory_peer(c, carry):
            rows_c = pl.ds(pl.multiple_of(c * ch, 8), ch)
            mem_send[rows_c, :] = memory_rows(pl.multiple_of(peer0 + c * ch, 8))
            mid_copy(mem_send, mem_recv, psend.at[0, c], precv.at[0, c], c).start()
            return carry

        lax.fori_loop(0, nch, memory_peer, 0)
        for k in range(2 * far):
            c_arrive(k).wait_recv()

        def own_terms(c, carry):
            rows_c = pl.ds(pl.multiple_of(c * ch, 8), ch)
            conv = conv_own[rows_c, :]
            mid_copy(conv_send, conv_recv, cvsend.at[c], cvrecv.at[c], c).wait()
            other = conv_recv[rows_c, :]
            memory = memory_rows(pl.multiple_of(own0 + c * ch, 8))
            for w0 in range(0, width, piece):
                cols = slice(w0, w0 + piece)
                acc[rows_c, cols] = (
                    jnp.dot(conv, vown[0:cw, cols], preferred_element_type=F32)
                    + jnp.dot(other, vother[0:cw, cols], preferred_element_type=F32)
                    + jnp.dot(memory, vown[cw : cw + vw, cols], preferred_element_type=F32)
                )
            return carry

        lax.fori_loop(0, nch, own_terms, 0)

        def last_terms(c, carry):
            rows_c = pl.ds(pl.multiple_of(c * ch, 8), ch)
            mid_copy(mem_send, mem_recv, psend.at[0, c], precv.at[0, c], c).wait()
            memory = mem_recv[rows_c, :]
            for w0 in range(0, width, piece):
                cols = slice(w0, w0 + piece)
                out[rows_c, cols] = (
                    acc[rows_c, cols]
                    + jnp.dot(memory, vother[cw : cw + vw, cols], preferred_element_type=F32)
                ).astype(BF)
            return carry

        lax.fori_loop(0, nch, last_terms, 0)
        cross.wait_send()
        for k in range(1, far):
            z_send(k).wait_send()
        for k in range(far):
            y_send(k).wait_send()
        for k in range(2 * far):
            c_send(k).wait_send()
        return

    def part_copy(k, c):
        spot = pl.ds(pl.multiple_of((k - 1) * own + c * ch, 8), ch)
        back = pl.ds(pl.multiple_of((n_tp - k - 1) * own + c * ch, 8), ch)
        return pltpu.make_async_remote_copy(
            src_ref=part_send.at[spot],
            dst_ref=part_recv.at[back],
            send_sem=psend.at[k - 1, c],
            recv_sem=precv.at[n_tp - k - 1, c],
            device_id={"tp": lax.rem(me + k, n_tp)},
            device_id_type=MESH,
        )

    def for_peer(step, carry):
        k = step // nch + 1
        c = step % nch
        owner = lax.rem(me + k, n_tp)
        finish(
            pl.multiple_of(owner * own + c * ch, 8), part_send, pl.multiple_of((k - 1) * own + c * ch, 8)
        )
        part_copy(k, c).start()
        return carry

    lax.fori_loop(0, (n_tp - 1) * nch, for_peer, 0)

    def for_self(c, carry):
        finish(pl.multiple_of(me * own + c * ch, 8), out, pl.multiple_of(c * ch, 8))
        return carry

    lax.fori_loop(0, nch, for_self, 0)

    def gather_parts(c, carry):
        spot = pl.ds(pl.multiple_of(c * ch, 8), ch)
        acc = out[spot, :].astype(F32)
        for k in range(1, n_tp):
            part_copy(k, c).wait_send()
            pltpu.make_async_remote_copy(
                src_ref=part_send.at[pl.ds(0, ch)],
                dst_ref=part_recv.at[pl.ds(pl.multiple_of((k - 1) * own + c * ch, 8), ch)],
                send_sem=psend.at[0, 0],
                recv_sem=precv.at[k - 1, c],
                device_id={"tp": lax.rem(me + k, n_tp)},
                device_id_type=MESH,
            ).wait_recv()
            acc = acc + part_recv[pl.ds(pl.multiple_of((k - 1) * own + c * ch, 8), ch), :].astype(F32)
        out[spot, :] = acc.astype(BF)
        return carry

    lax.fori_loop(0, nch, gather_parts, 0)


def on_device(n_sp, n_tp, *args):
    (tok, gain, wo, wi, ws, taps, wq, wk, wv, wg, gin, gfo, bin_, bfo, pos, extra, s0, p0, hgain, wco, wmo) = args
    own, width = tok.shape
    total = own * n_tp
    cw = wo.shape[1]
    qw = wq.shape[1]
    vw = wv.shape[1]
    heads = qw // DQK
    ch = 128 if own % 128 == 0 else own
    nch = own // ch
    rounds = n_sp.bit_length() - 1
    middle = exchanges_middle(n_sp, n_tp, own, cw, cw + vw)
    far = max(n_sp // 4, 1)
    vm = pl.BlockSpec(memory_space=pltpu.VMEM)
    hbm = pl.BlockSpec(memory_space=pl.ANY)
    weights = (2, 3, 4, 6, 7, 8, 9, 19, 20)
    V = pltpu.VMEM
    sem = pltpu.SemaphoreType.DMA
    return pl.pallas_call(
        functools.partial(kernel, n_sp, n_tp),
        out_shape=jax.ShapeDtypeStruct((own, width), BF),
        in_specs=[hbm if i in weights else vm for i in range(21)],
        out_specs=vm,
        scratch_shapes=[
            V((total, width), BF),
            V(wo.shape, BF), V(wi.shape, BF), V(ws.shape, BF), V(wq.shape, BF), V(wk.shape, BF),
            V(wv.shape, BF), V(wg.shape, BF), V((cw + vw, width), BF), V((cw + vw if middle else 16, width), BF),
            V((total, cw), BF), V((total + 8, cw), F32), V((total, qw), BF), V((total, qw), BF),
            V((total, vw), BF), V((total, vw), BF), V((total, 128), F32), V((128, total), F32),
            V((128, total), F32), V((total, 128), F32), V((total, vw), F32), V((8, cw), F32),
            V((rounds, heads, DQK, DV), BF), V((rounds, heads, DQK, DV), BF),
            V((rounds, 16, DV), F32), V((rounds, 16, DV), F32),
            V((heads, DQK, DV), BF), V((8, DV), F32),
            V((16 if middle else (n_tp - 1) * own, width), BF), V((16 if middle else (n_tp - 1) * own, width), BF),
            V((1, width), F32), V((hgain.shape[0] // DV, DV), F32),
            *[V((own if middle else 16, cw), BF)] * 3, *[V((own if middle else 16, vw), BF)] * 3,
            V((own if middle else 8, width), F32),
            sem((9,)), sem((n_tp - 1, nch)), sem((n_tp - 1, nch)), sem((2,)),
            sem((rounds, 2)), sem((rounds, 2)), sem((n_tp - 1, nch)), sem((n_tp - 1, nch)),
            sem((2,)), sem((far,)), sem((far,)), sem((far,)), sem((far,)), sem((2 * far,)), sem((2 * far,)), sem((nch,)), sem((nch,)),
        ],
        compiler_params=pltpu.CompilerParams(
            collective_id=0, has_side_effects=True, vmem_limit_bytes=62 * 1024 * 1024
        ),
    )(
        tok, gain.reshape(-1, 128), wo, wi, ws, taps, wq, wk, wv, wg, gin.T, gfo.T, bin_.reshape(1, -1),
        bfo.reshape(1, -1), pos.reshape(-1, 128), extra.T, s0, p0.reshape(1, -1), hgain.reshape(-1, DV), wco, wmo,
    )


def solution(mesh):
    cols = P(None, "tp")
    in_specs = (
        P(("sp", "tp"), None), P(), cols, cols, cols, P(), cols, cols, cols, cols, P(), P(), P(), P(),
        P("sp"), P("sp", None), P(), P(), P(), P("tp", None), P("tp", None),
    )
    body = functools.partial(on_device, mesh.shape["sp"], mesh.shape["tp"])
    return jax.shard_map(
        body, mesh=mesh, in_specs=in_specs, out_specs=P(("sp", "tp"), None), check_vma=False
    )
```
